32 devices in a mesh: gr: 2 (over y), sp: 4 (over z), tp: 4 (over x, core).
Axes of the slice: x: 2, y: 2, z: 4, core: 2. Of those that a mesh axis runs over, the one named last changes fastest.
Arguments:
- tokens: bfloat16 [8, 8192, 2048], P(('gr', 'tp'), 'sp'), may hold values from -6 to 6
- kv_weight: bfloat16 [2048, 1024], replicated, may hold values from -0.125 to 0.125
- queries: bfloat16 [8, 1536], P(('gr', 'tp')), may hold values from -6 to 6
- score_offset: float32 [24], replicated, may hold values from -10.5 to -3.5
Outputs:
- cache: bfloat16 [8, 4, 8192, 256], P(('gr', 'tp'), 'sp')
- read: bfloat16 [8, 1536], P(('gr', 'tp'))
The draws below stay inside these ranges and needn't reach their ends.
All inputs are finite; a program needn't handle non-finite values.
Results may differ from the reference program's by a relative error of at most 0.0085.
Values may be sent and summed in bfloat16 or wider, within the bound.
A program may use at most 64 MiB of HBM per device.

```python
import jax
import jax.numpy as jnp
from jax import lax

D = 2048
H = 24
KVH = 8
HD = 64
LEN = 8192
KVF = 1024
CB = 4
W = 256
SEQ_DEV = 1
GROUPS = 8
SEQS = 8
N_SP = 4


def levels(own_key, dims, pieces, low, top_value):
    def one(dim, parts):
        draws = jax.random.uniform(jax.random.fold_in(jax.random.fold_in(own_key, 6), dim), (parts,), jnp.float32, low / len(pieces), top_value / len(pieces))
        return jnp.repeat(jnp.exp(draws), dims[dim] // parts).reshape((-1,) + (1,) * (len(dims) - dim - 1))

    loudness = one(*pieces[0])
    for cut in pieces[1:]:
        loudness = loudness * one(*cut)
    return loudness


def bell_draw(own_key, dims, scale, reach, pieces=(), dtype=jnp.bfloat16):
    entries = scale * jax.random.normal(own_key, dims, jnp.float32)
    if pieces:
        entries = entries * levels(own_key, dims, pieces, -0.22, 0.18)
    return jnp.clip(entries, -reach, reach).astype(dtype)


def setup_inputs(seed: int = 0) -> dict:
    key_list = jax.random.split(jax.random.key(seed), 5)
    tokens = bell_draw(key_list[0], (SEQS, LEN, D), 1.0, 6.0, ((0, 8), (1, 4)))
    kv_weight = bell_draw(key_list[1], (D, KVF), D ** -0.5, 0.125)
    queries = bell_draw(key_list[2], (SEQS, H * HD), 1.0, 6.0, ((0, 8),))
    score_offset = jnp.clip(jax.random.uniform(key_list[3], (H,), jnp.float32, -10.5, -3.5), -10.5, -3.5)
    return dict(tokens=tokens, kv_weight=kv_weight, queries=queries, score_offset=score_offset)


def reference(tokens, kv_weight, queries, score_offset):
    projected = jnp.dot(tokens.reshape(SEQS * LEN, D), kv_weight, preferred_element_type=jnp.float32).astype(jnp.bfloat16)
    projected = projected.reshape(SEQS, LEN, KVF)
    cache = projected.reshape(GROUPS, SEQ_DEV, LEN, CB, W).transpose(0, 1, 3, 2, 4).reshape(GROUPS, N_SP, LEN, W)
    pairs = projected.reshape(SEQS, LEN, 2, KVH, HD)
    offsets = score_offset.reshape(KVH, H // KVH)

    def one_sequence(args):
        query_row, pair_rows = args
        query_heads = query_row.astype(jnp.float32).reshape(KVH, H // KVH, HD)
        key_rows = pair_rows[:, 0].astype(jnp.float32)
        value_rows = pair_rows[:, 1].astype(jnp.float32)
        logits = jnp.einsum('ngd,pnd->ngp', query_heads, key_rows) * (HD ** -0.5) + offsets[:, :, None]
        keep_log = jax.nn.log_sigmoid(-logits)
        between = lax.cumsum(keep_log, axis=2, reverse=True) - keep_log
        weights = jnp.exp(jax.nn.log_sigmoid(logits) + between)
        return jnp.einsum('ngp,pnd->ngd', weights, value_rows).reshape(H * HD)

    read = lax.map(one_sequence, (queries, pairs)).astype(jnp.bfloat16)
    return cache, read
```

```python
import functools

import jax
import jax.numpy as jnp
from jax import lax
from jax.experimental import pallas as pl
from jax.experimental.pallas import tpu as pltpu
from jax.sharding import PartitionSpec as P

KVH = 8
HD = 64


def prefix(shard, axis, combine, identity):
    size, index = (lax.axis_size(axis), lax.axis_index(axis))
    everything = lax.all_gather(shard, axis)
    start = jnp.broadcast_to(jnp.asarray(identity, shard.dtype), shard.shape)

    def hop(k, before):
        at = size - 1 - k
        reached = at > index
        new = combine(before, everything[at])
        return jnp.where(reached, new, before)

    return lax.fori_loop(0, size, hop, start)


def add_terms(earlier, later):
    return earlier + later


def finish(contribution):
    return lax.psum(contribution, "sp").astype(jnp.bfloat16)


def local_plain(tokens, kv_weight, queries, score_offset):
    seq_count, pos_rows, model_width = tokens.shape
    features = kv_weight.shape[1]
    slot_count = lax.axis_size("sp")
    blocks = slot_count // seq_count
    block_width = features // blocks
    half_blocks = blocks // 2
    heads = score_offset.shape[0]
    group_size = heads // KVH
    per_block = block_width // HD
    projected = jnp.einsum(
        "spd,dcw->scpw",
        tokens,
        kv_weight.reshape(model_width, blocks, block_width),
        preferred_element_type=jnp.float32,
    ).astype(jnp.bfloat16)
    received = lax.all_to_all(
        projected.reshape(slot_count, pos_rows, block_width),
        "sp",
        split_axis=0,
        concat_axis=1,
        tiled=True,
    )
    length = received.shape[1]
    cache = received.reshape(1, 1, length, block_width)
    key_part = projected[:, :half_blocks].reshape(seq_count, half_blocks, pos_rows, per_block, HD)
    value_part = (
        projected[:, half_blocks:]
        .reshape(seq_count, half_blocks, pos_rows, per_block, HD)
        .astype(jnp.float32)
    )
    query_heads = queries.reshape(seq_count, half_blocks, per_block, group_size, HD)
    offsets = score_offset.reshape(half_blocks, per_block, group_size)
    logits = jnp.einsum(
        "scvgd,scpvd->scvgp", query_heads, key_part, preferred_element_type=jnp.float32
    )
    logits = logits * HD ** (-0.5) + offsets[None, :, :, :, None]
    keep_log = jax.nn.log_sigmoid(-logits)
    between = lax.cumsum(keep_log, axis=4, reverse=True) - keep_log
    totals = jnp.sum(keep_log, axis=4)
    later_keep = prefix(totals, "sp", add_terms, jnp.zeros_like(totals))
    weights = jnp.exp(jax.nn.log_sigmoid(logits) + between + later_keep[..., None])
    weighted = jnp.einsum("scvgp,scpvd->scvgd", weights, value_part)
    contribution = weighted.reshape(seq_count, heads * HD)
    return (cache, finish(contribution))


CHUNK = 128
EARLY = 4
SLICES = 4
PLACES = 4
VMEM_LIMIT = 56 * 2**20
LANES = 128
MESH = pl.DeviceIdType.MESH


def exchange_kernel(
    count,
    tok_hbm,
    w_hbm,
    q_ref,
    off_ref,
    recv,
    read_ref,
    tok,
    wts,
    proj,
    qbig,
    part,
    whole,
    outer_part,
    other_part,
    inner_whole,
    tok_sem,
    w_sem,
    slice_sem,
    send_sem,
    recv_sem,
    psend_sem,
    precv_sem,
    ready,
    everyone,
):
    me = lax.axis_index("sp")
    rows = tok.shape[0]
    model_width = tok.shape[1]
    width = wts.shape[2]
    chunks = rows // CHUNK
    heads = off_ref.shape[1]
    group = heads // KVH
    half = count // 2
    depth = model_width // SLICES

    lower = me < half
    inner = jnp.where(lower, half - 1, half)
    mate = jnp.where(lower, half, half - 1)
    is_inner = me == inner
    inward = jnp.where(lower, me + 1, me - 1)
    outward = jnp.where(lower, me - 1, me + 1)
    has_outer = jnp.logical_and(me > 0, me < count - 1)

    def dest(j):
        if j == count - 1:
            return me
        down = count - 1 - j
        return jnp.where(
            lower,
            jnp.where(down > me, down, down - 1),
            jnp.where(j < me, j, j + 1),
        )

    def span(c):
        return pl.ds(pl.multiple_of(c * CHUNK, CHUNK), CHUNK)

    def tok_copy(c):
        return pltpu.make_async_copy(tok_hbm.at[span(c), :], tok.at[span(c), :], tok_sem.at[c])

    def w_copy(d):
        at = pl.ds(pl.multiple_of(d * width, width), width)
        return pltpu.make_async_copy(w_hbm.at[:, at], wts.at[d], w_sem.at[d])

    def slice_copy(k):
        at = pl.ds(pl.multiple_of(mate * width, width), width)
        deep = pl.ds(k * depth, depth)
        return pltpu.make_async_copy(
            w_hbm.at[deep, at], wts.at[mate, deep, :], slice_sem.at[k]
        )

    def block_copy(d, c):
        there = pl.ds(pl.multiple_of(me * rows + c * CHUNK, CHUNK), CHUNK)
        return pltpu.make_async_remote_copy(
            src_ref=proj.at[d, span(c), :],
            dst_ref=recv.at[there, :],
            send_sem=send_sem.at[d],
            recv_sem=recv_sem.at[me],
            device_id={"sp": d},
            device_id_type=MESH,
        )

    barrier = pltpu.get_barrier_semaphore()

    @pl.when(is_inner)
    def _():
        pl.semaphore_signal(barrier, inc=1, device_id={"sp": mate}, device_id_type=MESH)

    tok_copy(chunks - 1).start()
    for k in range(SLICES):
        slice_copy(k).start()

    first = jnp.zeros((CHUNK, width), jnp.float32)
    tok_copy(chunks - 1).wait()
    for k in range(SLICES):
        slice_copy(k).wait()
        if k == 0:
            tok_copy(chunks - 2).start()
            w_copy(dest(0)).start()
        deep = pl.ds(k * depth, depth)
        first = first + jnp.dot(
            tok[span(chunks - 1), deep], wts[mate, deep, :], preferred_element_type=jnp.float32
        )
    proj[mate, span(chunks - 1), :] = first.astype(jnp.bfloat16)
    for k in range(2, EARLY):
        tok_copy(chunks - 1 - k).start()
    for j in range(1, count):
        if j != half - 1:
            w_copy(dest(j)).start()
    pl.semaphore_wait(barrier, 1)
    block_copy(mate, chunks - 1).start()

    for d in range(count):
        same = (d < half) == lower

        @pl.when(jnp.logical_and(is_inner, jnp.logical_and(same, d != me)))
        def _():
            pl.semaphore_signal(barrier, inc=1, device_id={"sp": d}, device_id_type=MESH)

    @pl.when(jnp.logical_not(is_inner))
    def _():
        for d in (half - 1, half):
            pl.semaphore_signal(ready, inc=1, device_id={"sp": d}, device_id_type=MESH)

    def early(k, carry):
        c = chunks - 1 - k
        tok_copy(c).wait()
        proj[mate, span(c), :] = jnp.dot(
            tok[span(c), :], wts[mate], preferred_element_type=jnp.float32
        ).astype(jnp.bfloat16)

        @pl.when(k > 1)
        def _():
            block_copy(mate, c + 1).start()

        return carry

    lax.fori_loop(1, EARLY, early, 0)

    q_rows = []
    for h in range(heads):
        pair = q_ref[:, h // 2 * LANES : (h // 2 + 1) * LANES].astype(jnp.float32)
        q_rows.append(pair if h % 2 == h // group % 2 else pltpu.roll(pair, HD, axis=1))
    spread = jnp.concatenate(
        [jnp.concatenate(q_rows, axis=0)] * (KVH * HD // LANES), axis=1
    )
    diagonal = lax.broadcasted_iota(jnp.int32, (heads, LANES), 0) == lax.broadcasted_iota(
        jnp.int32, (heads, LANES), 1
    )

    def to_column(row):
        return jnp.sum(
            jnp.where(diagonal, jnp.broadcast_to(row, (heads, LANES)), 0.0), axis=1, keepdims=True
        )

    def to_row(column):
        return jnp.sum(
            jnp.where(diagonal, jnp.broadcast_to(column, (heads, LANES)), 0.0),
            axis=0,
            keepdims=True,
        )

    square = (heads, heads)
    offsets = jnp.sum(
        jnp.where(
            diagonal[:, :heads], jnp.broadcast_to(off_ref[...], square), 0.0
        ),
        axis=1,
        keepdims=True,
    )
    column = lax.broadcasted_iota(jnp.int32, spread.shape, 1) // HD
    row = lax.broadcasted_iota(jnp.int32, spread.shape, 0) // group
    mine = column == row
    qbig[...] = jnp.where(mine, spread, 0.0).astype(jnp.bfloat16)
    earlier = lax.broadcasted_iota(jnp.int32, (CHUNK, CHUNK), 1)
    later = lax.broadcasted_iota(jnp.int32, (CHUNK, CHUNK), 0)
    after = jnp.where(later > earlier, 1.0, 0.0).astype(jnp.bfloat16)

    block_copy(mate, chunks - EARLY).start()

    @pl.when(is_inner)
    def _():
        pl.semaphore_wait(ready, count - 2)

    for d in range(count):
        same = (d < half) == lower

        @pl.when(jnp.logical_and(is_inner, jnp.logical_and(same, d != me)))
        def _():
            pl.semaphore_signal(everyone, inc=1, device_id={"sp": d}, device_id_type=MESH)

    @pl.when(jnp.logical_not(is_inner))
    def _():
        pl.semaphore_wait(everyone, 1)

    def deferred(d):
        crosses = (d < half) != lower
        return jnp.logical_or(
            d == mate, jnp.logical_and(jnp.logical_not(crosses), jnp.logical_not(has_outer))
        )

    def step(i, state):
        kept, total = state
        c = chunks - 1 - i
        at = span(c)

        @pl.when(i >= EARLY)
        def _():
            tok_copy(c).wait()

        @pl.when(i + EARLY < chunks)
        def _():
            tok_copy(c - EARLY).start()

        before = None
        for j in range(count):
            d = dest(j)
            if j == half - 1:

                @pl.when(i >= EARLY)
                def _():
                    proj[mate, at, :] = jnp.dot(
                        tok[at, :], wts[mate], preferred_element_type=jnp.float32
                    ).astype(jnp.bfloat16)

            else:

                @pl.when(i == 0)
                def _():
                    w_copy(d).wait()

                block = jnp.dot(
                    tok[at, :], wts[d], preferred_element_type=jnp.float32
                ).astype(jnp.bfloat16)
                proj[d, at, :] = block
                if j == count - 1:
                    own = pl.ds(pl.multiple_of(me * rows + c * CHUNK, CHUNK), CHUNK)
                    recv[own, :] = block
            if before is not None:
                send = before

                @pl.when(jnp.logical_not(deferred(send)))
                def _():
                    block_copy(send, c).start()

            before = None if j == half - 1 else d

        logits = jnp.zeros((heads, CHUNK), jnp.float32)
        for b in range(half):
            logits = logits + lax.dot_general(
                qbig[:, b * width : (b + 1) * width],
                proj[b, at, :],
                (((1,), (1,)), ((), ())),
                preferred_element_type=jnp.float32,
            )
        logits = logits * HD ** (-0.5) + offsets
        keep = -(jnp.maximum(logits, 0.0) + jnp.log1p(jnp.exp(-jnp.abs(logits))))
        high = keep.astype(jnp.bfloat16)
        rest = keep - high.astype(jnp.float32)
        mid = rest.astype(jnp.bfloat16)
        low = (rest - mid.astype(jnp.float32)).astype(jnp.bfloat16)
        sums = jnp.dot(
            jnp.concatenate([high, mid, low], axis=0), after, preferred_element_type=jnp.float32
        )
        between = sums[:heads] + sums[heads : 2 * heads] + sums[2 * heads :]
        weight = jnp.exp(logits + keep + between + kept)
        weight_high = weight.astype(jnp.bfloat16)
        weight_low = (weight - weight_high.astype(jnp.float32)).astype(jnp.bfloat16)
        both = jnp.concatenate([weight_high, weight_low], axis=0)
        summed = jnp.concatenate(
            [
                jnp.dot(both, proj[half + b, at, :], preferred_element_type=jnp.float32)
                for b in range(half)
            ],
            axis=1,
        )
        total = total + summed[:heads] + summed[heads:]
        kept = kept + jnp.sum(keep, axis=1, keepdims=True)
        return kept, total

    kept, total = lax.fori_loop(
        0,
        chunks,
        step,
        (jnp.zeros((heads, 1), jnp.float32), jnp.zeros((heads, KVH * HD), jnp.float32)),
    )

    pairs = heads // 2
    left_lanes = lax.broadcasted_iota(jnp.int32, (heads, LANES), 1) < HD
    left_head = lax.broadcasted_iota(jnp.int32, (heads, LANES), 0) // group % 2 == 0

    def pack(x):
        x = jnp.where(left_lanes == left_head, x, 0.0)
        return jnp.concatenate(
            [
                x[2 * g * group : (2 * g + 1) * group] + x[(2 * g + 1) * group : (2 * g + 2) * group]
                for g in range(KVH // 2)
            ],
            axis=0,
        )

    def join(early_sums, early_row, late_sums, late_row):
        spread_keep = jnp.broadcast_to(to_column(late_row), (heads, LANES))
        return late_sums + jnp.exp(pack(spread_keep)) * early_sums, early_row + late_row

    def join_sides(sums, row, other_sums, other_row, own_late):
        return join(
            jnp.where(own_late, other_sums, sums),
            jnp.where(own_late, other_row, row),
            jnp.where(own_late, sums, other_sums),
            jnp.where(own_late, row, other_row),
        )

    total = jnp.where(mine, total, 0.0)
    folded = total[:, :LANES]
    for g in range(1, KVH * HD // LANES):
        folded = folded + total[:, g * LANES : (g + 1) * LANES]
    part[:pairs] = pack(folded)
    part[pairs:] = to_row(kept)

    def part_copy(src, dst, to, sent, got):
        return pltpu.make_async_remote_copy(
            src_ref=src,
            dst_ref=dst,
            send_sem=psend_sem.at[sent],
            recv_sem=precv_sem.at[got],
            device_id={"sp": to},
            device_id_type=MESH,
        )

    def send_deferred(start, stop):
        @pl.loop(start, stop)
        def _(i):
            for j in range(count - 1):
                d = dest(j)
                ahead = i >= EARLY if j == half - 1 else True

                @pl.when(jnp.logical_and(deferred(d), ahead))
                def _():
                    block_copy(d, chunks - 1 - i).start()

    pause = 2 * EARLY if chunks > 2 * EARLY else chunks

    @pl.when(has_outer)
    def _():
        send_deferred(EARLY, pause)
        part_copy(part, outer_part, inward, 0, 0).wait_recv()
        sums, row = join_sides(
            part[:pairs], part[pairs:], outer_part[:pairs], outer_part[pairs:], lower
        )
        part[:pairs] = sums
        part[pairs:] = row

    @pl.when(jnp.logical_not(has_outer))
    def _():
        send_deferred(0, EARLY)

    @pl.when(is_inner)
    def _():
        part_copy(part, other_part, mate, 0, 1).start()

    @pl.when(jnp.logical_not(is_inner))
    def _():
        part_copy(part, outer_part, inward, 0, 0).start()

    @pl.when(has_outer)
    def _():
        send_deferred(pause, chunks)

    @pl.when(jnp.logical_not(has_outer))
    def _():
        send_deferred(EARLY, chunks)

    @pl.when(is_inner)
    def _():
        part_copy(part, other_part, mate, 0, 1).wait_recv()
        sums, row = join_sides(
            part[:pairs],
            part[pairs:],
            other_part[:pairs],
            other_part[pairs:],
            jnp.logical_not(lower),
        )
        whole[:pairs] = sums
        whole[pairs:] = row

    @pl.when(jnp.logical_not(is_inner))
    def _():
        part_copy(whole, inner_whole, outward, 1, 2).wait_recv()
        whole[...] = inner_whole[...]

    packed = whole[:pairs]
    turned = pltpu.roll(packed, HD, axis=1)
    low_half = lax.broadcasted_iota(jnp.int32, (1, LANES), 1) < HD

    def head_at(h, side):
        source = packed if h // group % 2 == side else turned
        at = h // group // 2 * group + h % group
        return source[at : at + 1]

    for m in range(pairs):
        piece = jnp.where(low_half, head_at(2 * m, 0), head_at(2 * m + 1, 1))
        read_ref[:, m * LANES : (m + 1) * LANES] = piece.astype(read_ref.dtype)

    @pl.when(has_outer)
    def _():
        out = part_copy(whole, inner_whole, outward, 1, 2)
        out.start()
        out.wait_send()

    part_copy(part, other_part, mate, 0, 1).wait_send()
    for j in range(count - 2, -1, -1):
        d = dest(j)
        copy = pltpu.make_async_remote_copy(
            src_ref=proj.at[d],
            dst_ref=recv.at[pl.ds(pl.multiple_of(d * rows, CHUNK), rows), :],
            send_sem=send_sem.at[d],
            recv_sem=recv_sem.at[d],
            device_id={"sp": d},
            device_id_type=MESH,
        )
        copy.wait()


def place_kernel(got, read, cache, read_out, sems):
    rows = got.shape[0] // PLACES
    copies = []
    for k in range(PLACES):
        at = pl.ds(k * rows, rows)
        copies.append(pltpu.make_async_copy(got.at[at, :], cache.at[at, :], sems.at[k]))
    copies.append(pltpu.make_async_copy(read, read_out, sems.at[PLACES]))
    for copy in copies:
        copy.start()
    for copy in copies:
        copy.wait()


def local(tokens, kv_weight, queries, score_offset):
    seq_count, rows, model_width = tokens.shape
    features = kv_weight.shape[1]
    heads = score_offset.shape[0]
    count = lax.axis_size("sp")
    width = features // (count // seq_count)
    fits = (
        seq_count == 1
        and count % 2 == 0
        and count > 2
        and width % LANES == 0
        and rows % CHUNK == 0
        and rows > EARLY * CHUNK
        and model_width % (SLICES * LANES) == 0
        and features == 2 * KVH * HD
        and 2 * HD == LANES
        and heads % KVH == 0
        and heads <= LANES
    )
    if not fits:
        return local_plain(tokens, kv_weight, queries, score_offset)
    length = rows * count
    vmem = pl.BlockSpec(memory_space=pltpu.VMEM)
    hbm = pl.BlockSpec(memory_space=pltpu.HBM)
    got, read = pl.pallas_call(
        functools.partial(exchange_kernel, count),
        out_shape=(
            pltpu.VMEM((length, width), jnp.bfloat16),
            pltpu.VMEM((1, heads * HD), jnp.bfloat16),
        ),
        in_specs=[hbm, hbm, vmem, vmem],
        out_specs=(vmem, vmem),
        scratch_shapes=[
            pltpu.VMEM((rows, model_width), jnp.bfloat16),
            pltpu.VMEM((count, model_width, width), jnp.bfloat16),
            pltpu.VMEM((count, rows, width), jnp.bfloat16),
            pltpu.VMEM((heads, KVH * HD), jnp.bfloat16),
            *[pltpu.VMEM((heads // 2 + 1, LANES), jnp.float32)] * 5,
            pltpu.SemaphoreType.DMA((rows // CHUNK,)),
            pltpu.SemaphoreType.DMA((count,)),
            pltpu.SemaphoreType.DMA((SLICES,)),
            pltpu.SemaphoreType.DMA((count,)),
            pltpu.SemaphoreType.DMA((count,)),
            pltpu.SemaphoreType.DMA((2,)),
            pltpu.SemaphoreType.DMA((3,)),
            pltpu.SemaphoreType.REGULAR,
            pltpu.SemaphoreType.REGULAR,
        ],
        compiler_params=pltpu.CompilerParams(
            collective_id=0, has_side_effects=True, vmem_limit_bytes=VMEM_LIMIT
        ),
    )(
        tokens.reshape(rows, model_width),
        kv_weight,
        queries,
        score_offset.reshape(1, heads),
    )
    cache, read = pl.pallas_call(
        place_kernel,
        out_shape=(
            jax.ShapeDtypeStruct((length, width), jnp.bfloat16),
            jax.ShapeDtypeStruct((1, heads * HD), jnp.bfloat16),
        ),
        in_specs=[vmem, vmem],
        out_specs=(hbm, hbm),
        scratch_shapes=[pltpu.SemaphoreType.DMA((PLACES + 1,))],
        compiler_params=pltpu.CompilerParams(vmem_limit_bytes=8 * 2**20),
    )(got, read)
    return cache.reshape(1, 1, length, width), read


def solution(mesh):
    placed = (P(("gr", "tp"), "sp", None), P(), P(("gr", "tp"), None), P())
    return jax.shard_map(
        local,
        mesh=mesh,
        in_specs=placed,
        out_specs=(P(("gr", "tp"), "sp", None, None), P(("gr", "tp"), None)),
        check_vma=False,
    )
```

```python
import functools

import jax
import jax.numpy as jnp
from jax import lax
from jax.experimental import pallas as pl
from jax.experimental.pallas import tpu as pltpu
from jax.sharding import PartitionSpec as P

KVH = 8
HD = 64


def prefix(shard, axis, combine, identity):
    size, index = (lax.axis_size(axis), lax.axis_index(axis))
    everything = lax.all_gather(shard, axis)
    start = jnp.broadcast_to(jnp.asarray(identity, shard.dtype), shard.shape)

    def hop(k, before):
        at = size - 1 - k
        reached = at > index
        new = combine(before, everything[at])
        return jnp.where(reached, new, before)

    return lax.fori_loop(0, size, hop, start)


def add_terms(earlier, later):
    return earlier + later


def finish(contribution):
    return lax.psum(contribution, "sp").astype(jnp.bfloat16)


def local_plain(tokens, kv_weight, queries, score_offset):
    seq_count, pos_rows, model_width = tokens.shape
    features = kv_weight.shape[1]
    slot_count = lax.axis_size("sp")
    blocks = slot_count // seq_count
    block_width = features // blocks
    half_blocks = blocks // 2
    heads = score_offset.shape[0]
    group_size = heads // KVH
    per_block = block_width // HD
    projected = jnp.einsum(
        "spd,dcw->scpw",
        tokens,
        kv_weight.reshape(model_width, blocks, block_width),
        preferred_element_type=jnp.float32,
    ).astype(jnp.bfloat16)
    received = lax.all_to_all(
        projected.reshape(slot_count, pos_rows, block_width),
        "sp",
        split_axis=0,
        concat_axis=1,
        tiled=True,
    )
    length = received.shape[1]
    cache = received.reshape(1, 1, length, block_width)
    key_part = projected[:, :half_blocks].reshape(seq_count, half_blocks, pos_rows, per_block, HD)
    value_part = (
        projected[:, half_blocks:]
        .reshape(seq_count, half_blocks, pos_rows, per_block, HD)
        .astype(jnp.float32)
    )
    query_heads = queries.reshape(seq_count, half_blocks, per_block, group_size, HD)
    offsets = score_offset.reshape(half_blocks, per_block, group_size)
    logits = jnp.einsum(
        "scvgd,scpvd->scvgp", query_heads, key_part, preferred_element_type=jnp.float32
    )
    logits = logits * HD ** (-0.5) + offsets[None, :, :, :, None]
    keep_log = jax.nn.log_sigmoid(-logits)
    between = lax.cumsum(keep_log, axis=4, reverse=True) - keep_log
    totals = jnp.sum(keep_log, axis=4)
    later_keep = prefix(totals, "sp", add_terms, jnp.zeros_like(totals))
    weights = jnp.exp(jax.nn.log_sigmoid(logits) + between + later_keep[..., None])
    weighted = jnp.einsum("scvgp,scpvd->scvgd", weights, value_part)
    contribution = weighted.reshape(seq_count, heads * HD)
    return (cache, finish(contribution))


CHUNK = 128
FIRST = 64
EARLY = 4
SLICES = 4
LATE = 12
VMEM_LIMIT = 51 * 2**20
LANES = 128
MESH = pl.DeviceIdType.MESH


def is_late(count):
    me = lax.axis_index("sp")
    in_middle = jnp.logical_or(me == count // 2 - 1, me == count // 2)
    return jnp.logical_and(in_middle, lax.rem(lax.axis_index("tp"), 2) == 1)


def exchange_kernel(
    count,
    tok_hbm,
    w_hbm,
    q_hbm,
    off_hbm,
    recv,
    read_ref,
    proj,
    tok,
    wts,
    q_ref,
    off_ref,
    qbig,
    part,
    whole,
    outer_part,
    other_part,
    inner_whole,
    load_sem,
    send_sem,
    recv_sem,
    psend_sem,
    precv_sem,
    ready,
):
    me = lax.axis_index("sp")
    rows = tok.shape[0]
    model_width = tok.shape[1]
    width = wts.shape[2]
    chunks = rows // CHUNK
    heads = off_ref.shape[1]
    group = heads // KVH
    half = count // 2
    depth = model_width // SLICES

    lower = me < half
    inner = jnp.where(lower, half - 1, half)
    mate = jnp.where(lower, half, half - 1)
    is_inner = me == inner
    inward = jnp.where(lower, me + 1, me - 1)
    outward = jnp.where(lower, me - 1, me + 1)
    has_outer = jnp.logical_and(me > 0, me < count - 1)

    def dest(j):
        if j == count - 1:
            return me
        down = count - 1 - j
        return jnp.where(
            lower,
            jnp.where(down > me, down, down - 1),
            jnp.where(j < me, j, j + 1),
        )

    def span(c):
        return pl.ds(pl.multiple_of(c * CHUNK, CHUNK), CHUNK)

    def tok_copy(c):
        sem = load_sem.at[lax.rem(c, EARLY)]
        return pltpu.make_async_copy(tok_hbm.at[span(c), :], tok.at[span(c), :], sem)

    def w_copy(d):
        at = pl.ds(pl.multiple_of(d * width, width), width)
        return pltpu.make_async_copy(w_hbm.at[:, at], wts.at[d], load_sem.at[EARLY + 2])

    def slice_copy(k):
        at = pl.ds(pl.multiple_of(mate * width, width), width)
        deep = pl.ds(k * depth, depth)
        return pltpu.make_async_copy(
            w_hbm.at[deep, at], wts.at[mate, deep, :], load_sem.at[EARLY + k]
        )

    def rows_copy(d, start, size):
        here = pl.ds(pl.multiple_of(start, FIRST), size)
        there = pl.ds(pl.multiple_of(me * rows + start, FIRST), size)
        return pltpu.make_async_remote_copy(
            src_ref=proj.at[d, here, :],
            dst_ref=recv.at[there, :],
            send_sem=send_sem,
            recv_sem=recv_sem,
            device_id={"sp": d},
            device_id_type=MESH,
        )

    def block_copy(d, c):
        return rows_copy(d, c * CHUNK, CHUNK)

    def top_copy(start, size, sem):
        at = pl.ds(start, size)
        return pltpu.make_async_copy(tok_hbm.at[at, :], tok.at[at, :], load_sem.at[sem])

    barrier = pltpu.get_barrier_semaphore()

    @pl.when(is_inner)
    def _():
        pl.semaphore_signal(barrier, inc=1, device_id={"sp": mate}, device_id_type=MESH)

    first_at, rest_at = rows - FIRST, rows - CHUNK
    first_copy = top_copy(first_at, FIRST, EARLY + SLICES)
    rest_copy = top_copy(rest_at, CHUNK - FIRST, (chunks - 1) % EARLY)
    first_copy.start()
    for k in range(SLICES):
        slice_copy(k).start()
    rest_copy.start()
    tok_copy(chunks - 2).start()

    first = jnp.zeros((FIRST, width), jnp.float32)
    first_copy.wait()
    for k in range(SLICES):
        slice_copy(k).wait()
        if k == 0:
            for early_chunk in range(2, EARLY):
                tok_copy(chunks - 1 - early_chunk).start()
        deep = pl.ds(k * depth, depth)
        first = first + jnp.dot(
            tok[pl.ds(first_at, FIRST), deep], wts[mate, deep, :], preferred_element_type=jnp.float32
        )
    proj[mate, pl.ds(first_at, FIRST), :] = first.astype(jnp.bfloat16)
    small_copies = [
        pltpu.make_async_copy(q_hbm, q_ref, load_sem.at[EARLY]),
        pltpu.make_async_copy(off_hbm, off_ref, load_sem.at[EARLY + 1]),
    ]
    for j in range(count):
        if j != half - 1:
            w_copy(dest(j)).start()
    for copy in small_copies:
        copy.start()
    pl.semaphore_wait(barrier, 1)
    rows_copy(mate, first_at, FIRST).start()

    for d in range(count):
        same = (d < half) == lower

        @pl.when(jnp.logical_and(is_inner, jnp.logical_and(same, d != me)))
        def _():
            pl.semaphore_signal(barrier, inc=1, device_id={"sp": d}, device_id_type=MESH)

    @pl.when(jnp.logical_not(is_inner))
    def _():
        for d in (half - 1, half):
            pl.semaphore_signal(ready, inc=1, device_id={"sp": d}, device_id_type=MESH)

    rest_copy.wait()
    proj[mate, pl.ds(rest_at, CHUNK - FIRST), :] = jnp.dot(
        tok[pl.ds(rest_at, CHUNK - FIRST), :], wts[mate], preferred_element_type=jnp.float32
    ).astype(jnp.bfloat16)

    def early(k, carry):
        c = chunks - 1 - k
        tok_copy(c).wait()
        proj[mate, span(c), :] = jnp.dot(
            tok[span(c), :], wts[mate], preferred_element_type=jnp.float32
        ).astype(jnp.bfloat16)

        @pl.when(k == 1)
        def _():
            rows_copy(mate, rest_at, CHUNK - FIRST).start()

        @pl.when(k > 1)
        def _():
            block_copy(mate, c + 1).start()

        return carry

    lax.fori_loop(1, EARLY, early, 0)
    for copy in small_copies:
        copy.wait()

    q_rows = []
    for h in range(heads):
        pair = q_ref[:, h // 2 * LANES : (h // 2 + 1) * LANES].astype(jnp.float32)
        q_rows.append(pair if h % 2 == h // group % 2 else pltpu.roll(pair, HD, axis=1))
    spread = jnp.concatenate(
        [jnp.concatenate(q_rows, axis=0)] * (KVH * HD // LANES), axis=1
    )
    diagonal = lax.broadcasted_iota(jnp.int32, (heads, LANES), 0) == lax.broadcasted_iota(
        jnp.int32, (heads, LANES), 1
    )

    def to_column(row):
        return jnp.sum(
            jnp.where(diagonal, jnp.broadcast_to(row, (heads, LANES)), 0.0), axis=1, keepdims=True
        )

    def to_row(column):
        return jnp.sum(
            jnp.where(diagonal, jnp.broadcast_to(column, (heads, LANES)), 0.0),
            axis=0,
            keepdims=True,
        )

    square = (heads, heads)
    offsets = jnp.sum(
        jnp.where(
            diagonal[:, :heads], jnp.broadcast_to(off_ref[...], square), 0.0
        ),
        axis=1,
        keepdims=True,
    )
    column = lax.broadcasted_iota(jnp.int32, spread.shape, 1) // HD
    row = lax.broadcasted_iota(jnp.int32, spread.shape, 0) // group
    mine = column == row
    qbig[...] = jnp.where(mine, spread, 0.0).astype(jnp.bfloat16)
    earlier = lax.broadcasted_iota(jnp.int32, (CHUNK, CHUNK), 1)
    later = lax.broadcasted_iota(jnp.int32, (CHUNK, CHUNK), 0)
    after = jnp.where(later > earlier, 1.0, 0.0).astype(jnp.bfloat16)

    block_copy(mate, chunks - EARLY).start()

    @pl.when(is_inner)
    def _():
        pl.semaphore_wait(ready, count - 2)

    for d in range(count):
        same = (d < half) == lower

        @pl.when(jnp.logical_and(is_inner, jnp.logical_and(same, d != me)))
        def _():
            pl.semaphore_signal(ready, inc=1, device_id={"sp": d}, device_id_type=MESH)

    @pl.when(jnp.logical_not(is_inner))
    def _():
        pl.semaphore_wait(ready, 1)

    others = pl.ds(0, count - 1)
    pltpu.make_async_copy(wts.at[others], wts.at[others], load_sem.at[EARLY + 2]).wait()

    def deferred(d):
        crosses = (d < half) != lower
        return jnp.logical_or(
            d == mate, jnp.logical_and(jnp.logical_not(crosses), jnp.logical_not(has_outer))
        )

    def step(i, state):
        kept, total = state
        c = chunks - 1 - i
        at = span(c)

        @pl.when(i >= EARLY)
        def _():
            tok_copy(c).wait()

        @pl.when(i + EARLY < chunks)
        def _():
            tok_copy(c - EARLY).start()

        before = None
        for j in range(count):
            d = dest(j)
            if j == half - 1:

                @pl.when(i >= EARLY)
                def _():
                    proj[mate, at, :] = jnp.dot(
                        tok[at, :], wts[mate], preferred_element_type=jnp.float32
                    ).astype(jnp.bfloat16)

            else:

                block = jnp.dot(
                    tok[at, :], wts[d], preferred_element_type=jnp.float32
                ).astype(jnp.bfloat16)
                proj[d, at, :] = block
                if j == count - 1:
                    own = pl.ds(pl.multiple_of(me * rows + c * CHUNK, CHUNK), CHUNK)
                    recv[own, :] = block
            if before is not None:
                send = before

                @pl.when(jnp.logical_not(deferred(send)))
                def _():
                    block_copy(send, c).start()

            before = None if j == half - 1 else d

        logits = jnp.zeros((heads, CHUNK), jnp.float32)
        for b in range(half):
            logits = logits + lax.dot_general(
                qbig[:, b * width : (b + 1) * width],
                proj[b, at, :],
                (((1,), (1,)), ((), ())),
                preferred_element_type=jnp.float32,
            )
        logits = logits * HD ** (-0.5) + offsets
        keep = -(jnp.maximum(logits, 0.0) + jnp.log1p(jnp.exp(-jnp.abs(logits))))
        high = keep.astype(jnp.bfloat16)
        rest = keep - high.astype(jnp.float32)
        mid = rest.astype(jnp.bfloat16)
        low = (rest - mid.astype(jnp.float32)).astype(jnp.bfloat16)
        sums = jnp.dot(
            jnp.concatenate([high, mid, low], axis=0), after, preferred_element_type=jnp.float32
        )
        between = sums[:heads] + sums[heads : 2 * heads] + sums[2 * heads :]
        weight = jnp.exp(logits + keep + between + kept)
        weight_high = weight.astype(jnp.bfloat16)
        weight_low = (weight - weight_high.astype(jnp.float32)).astype(jnp.bfloat16)
        both = jnp.concatenate([weight_high, weight_low], axis=0)
        summed = jnp.concatenate(
            [
                jnp.dot(both, proj[half + b, at, :], preferred_element_type=jnp.float32)
                for b in range(half)
            ],
            axis=1,
        )
        total = total + summed[:heads] + summed[heads:]
        kept = kept + jnp.sum(keep, axis=1, keepdims=True)
        return kept, total

    kept, total = lax.fori_loop(
        0,
        chunks,
        step,
        (jnp.zeros((heads, 1), jnp.float32), jnp.zeros((heads, KVH * HD), jnp.float32)),
    )

    pairs = heads // 2
    left_lanes = lax.broadcasted_iota(jnp.int32, (heads, LANES), 1) < HD
    left_head = lax.broadcasted_iota(jnp.int32, (heads, LANES), 0) // group % 2 == 0

    def pack(x):
        x = jnp.where(left_lanes == left_head, x, 0.0)
        return jnp.concatenate(
            [
                x[2 * g * group : (2 * g + 1) * group] + x[(2 * g + 1) * group : (2 * g + 2) * group]
                for g in range(KVH // 2)
            ],
            axis=0,
        )

    def join(early_sums, early_row, late_sums, late_row):
        spread_keep = jnp.broadcast_to(to_column(late_row), (heads, LANES))
        return late_sums + jnp.exp(pack(spread_keep)) * early_sums, early_row + late_row

    def join_sides(sums, row, other_sums, other_row, own_late):
        return join(
            jnp.where(own_late, other_sums, sums),
            jnp.where(own_late, other_row, row),
            jnp.where(own_late, sums, other_sums),
            jnp.where(own_late, row, other_row),
        )

    total = jnp.where(mine, total, 0.0)
    folded = total[:, :LANES]
    for g in range(1, KVH * HD // LANES):
        folded = folded + total[:, g * LANES : (g + 1) * LANES]
    part[:pairs] = pack(folded)
    part[pairs:] = to_row(kept)

    def part_copy(src, dst, to, sent, got):
        return pltpu.make_async_remote_copy(
            src_ref=src,
            dst_ref=dst,
            send_sem=psend_sem.at[sent],
            recv_sem=precv_sem.at[got],
            device_id={"sp": to},
            device_id_type=MESH,
        )

    def send_deferred(start, stop):
        @pl.loop(start, stop)
        def _(i):
            for j in range(count - 1):
                d = dest(j)
                ahead = i >= EARLY if j == half - 1 else True

                @pl.when(jnp.logical_and(deferred(d), ahead))
                def _():
                    block_copy(d, chunks - 1 - i).start()

    late = is_late(count)
    stop = jnp.where(late, chunks - LATE, chunks)
    pause = jnp.minimum(2 * EARLY, stop)

    @pl.when(has_outer)
    def _():
        send_deferred(EARLY, pause)
        part_copy(part, outer_part, inward, 0, 0).wait_recv()
        sums, row = join_sides(
            part[:pairs], part[pairs:], outer_part[:pairs], outer_part[pairs:], lower
        )
        part[:pairs] = sums
        part[pairs:] = row

    @pl.when(jnp.logical_not(has_outer))
    def _():
        send_deferred(0, EARLY)

    @pl.when(is_inner)
    def _():
        part_copy(part, other_part, mate, 0, 1).start()

    @pl.when(jnp.logical_not(is_inner))
    def _():
        part_copy(part, outer_part, inward, 0, 0).start()

    @pl.when(has_outer)
    def _():
        send_deferred(pause, stop)

    @pl.when(jnp.logical_not(has_outer))
    def _():
        send_deferred(EARLY, chunks)

    @pl.when(is_inner)
    def _():
        part_copy(part, other_part, mate, 0, 1).wait_recv()
        sums, row = join_sides(
            part[:pairs],
            part[pairs:],
            other_part[:pairs],
            other_part[pairs:],
            jnp.logical_not(lower),
        )
        whole[:pairs] = sums
        whole[pairs:] = row

    @pl.when(jnp.logical_not(is_inner))
    def _():
        part_copy(whole, inner_whole, outward, 1, 1).wait_recv()
        whole[...] = inner_whole[...]

    packed = whole[:pairs]
    turned = pltpu.roll(packed, HD, axis=1)
    low_half = lax.broadcasted_iota(jnp.int32, (1, LANES), 1) < HD

    def head_at(h, side):
        source = packed if h // group % 2 == side else turned
        at = h // group // 2 * group + h % group
        return source[at : at + 1]

    for m in range(pairs):
        piece = jnp.where(low_half, head_at(2 * m, 0), head_at(2 * m + 1, 1))
        read_ref[:, m * LANES : (m + 1) * LANES] = piece.astype(read_ref.dtype)

    @pl.when(has_outer)
    def _():
        out = part_copy(whole, inner_whole, outward, 1, 1)
        out.start()
        out.wait_send()

    part_copy(part, other_part, mate, 0, 1).wait_send()
    def finish_blocks(size):
        foreign = pl.ds(0, size)
        blocks = pltpu.make_async_remote_copy(
            src_ref=recv.at[foreign, :],
            dst_ref=recv.at[foreign, :],
            send_sem=send_sem,
            recv_sem=recv_sem,
            device_id={"sp": mate},
            device_id_type=MESH,
        )
        blocks.wait_send()
        blocks.wait_recv()

    @pl.when(late)
    def _():
        finish_blocks((count - 1) * rows - LATE * CHUNK)

    @pl.when(jnp.logical_not(late))
    def _():
        finish_blocks((count - 1) * rows)


def second_kernel(count, proj, _, rest, send_sem, recv_sem):
    me = lax.axis_index("sp")
    mate = jnp.where(me < count // 2, count // 2, count // 2 - 1)

    @pl.when(is_late(count))
    def _():
        barrier = pltpu.get_barrier_semaphore()
        pl.semaphore_signal(barrier, inc=1, device_id={"sp": mate}, device_id_type=MESH)
        pl.semaphore_wait(barrier, 1)
        copy = pltpu.make_async_remote_copy(
            src_ref=proj.at[mate, pl.ds(0, LATE * CHUNK), :],
            dst_ref=rest,
            send_sem=send_sem,
            recv_sem=recv_sem,
            device_id={"sp": mate},
            device_id_type=MESH,
        )
        copy.start()
        copy.wait()


def place_kernel(count, got, read, cache, read_out, sem, read_sem):
    rows = got.shape[0] // count
    me = lax.axis_index("sp")
    mate = jnp.where(me < count // 2, count // 2, count // 2 - 1)
    late = is_late(count)

    def copy(start, size):
        at = pl.ds(pl.multiple_of(start, CHUNK), size)
        return pltpu.make_async_copy(got.at[at, :], cache.at[at, :], sem)

    read_copy = pltpu.make_async_copy(read, read_out, read_sem)
    for d in range(count):

        @pl.when(jnp.logical_and(late, d == mate))
        def _():
            copy(d * rows + LATE * CHUNK, rows - LATE * CHUNK).start()

        @pl.when(jnp.logical_not(jnp.logical_and(late, d == mate)))
        def _():
            copy(d * rows, rows).start()

    read_copy.start()
    read_copy.wait()

    @pl.when(late)
    def _():
        copy(0, count * rows - LATE * CHUNK).wait()

    @pl.when(jnp.logical_not(late))
    def _():
        copy(0, count * rows).wait()


def complete_kernel(count, rest, _, cache, sem):
    rows = cache.shape[0] // count
    me = lax.axis_index("sp")
    mate = jnp.where(me < count // 2, count // 2, count // 2 - 1)

    @pl.when(is_late(count))
    def _():
        at = pl.ds(pl.multiple_of(mate * rows, CHUNK), LATE * CHUNK)
        copy = pltpu.make_async_copy(rest, cache.at[at, :], sem)
        copy.start()
        copy.wait()


def local(tokens, kv_weight, queries, score_offset):
    seq_count, rows, model_width = tokens.shape
    features = kv_weight.shape[1]
    heads = score_offset.shape[0]
    count = lax.axis_size("sp")
    width = features // (count // seq_count)
    fits = (
        seq_count == 1
        and count % 2 == 0
        and count > 2
        and width % LANES == 0
        and rows % CHUNK == 0
        and rows >= (EARLY + LATE) * CHUNK
        and model_width % (SLICES * LANES) == 0
        and features == 2 * KVH * HD
        and 2 * HD == LANES
        and heads % KVH == 0
        and rows // CHUNK % EARLY == 0
        and heads <= LANES
    )
    if not fits:
        return local_plain(tokens, kv_weight, queries, score_offset)
    length = rows * count
    vmem = pl.BlockSpec(memory_space=pltpu.VMEM)
    hbm = pl.BlockSpec(memory_space=pltpu.HBM)
    got, read, proj = pl.pallas_call(
        functools.partial(exchange_kernel, count),
        out_shape=(
            pltpu.VMEM((length, width), jnp.bfloat16),
            pltpu.VMEM((1, heads * HD), jnp.bfloat16),
            pltpu.VMEM((count, rows, width), jnp.bfloat16),
        ),
        in_specs=[hbm, hbm, hbm, hbm],
        out_specs=(vmem, vmem, vmem),
        scratch_shapes=[
            pltpu.VMEM((rows, model_width), jnp.bfloat16),
            pltpu.VMEM((count, model_width, width), jnp.bfloat16),
            pltpu.VMEM((1, heads * HD), jnp.bfloat16),
            pltpu.VMEM((1, heads), jnp.float32),
            pltpu.VMEM((heads, KVH * HD), jnp.bfloat16),
            *[pltpu.VMEM((heads // 2 + 1, LANES), jnp.float32)] * 5,
            pltpu.SemaphoreType.DMA((EARLY + SLICES + 1,)),
            pltpu.SemaphoreType.DMA,
            pltpu.SemaphoreType.DMA,
            pltpu.SemaphoreType.DMA((2,)),
            pltpu.SemaphoreType.DMA((2,)),
            pltpu.SemaphoreType.REGULAR,
        ],
        compiler_params=pltpu.CompilerParams(
            collective_id=0, has_side_effects=True, vmem_limit_bytes=VMEM_LIMIT
        ),
    )(
        tokens.reshape(rows, model_width),
        kv_weight,
        queries,
        score_offset.reshape(1, heads),
    )
    cache, read = pl.pallas_call(
        functools.partial(place_kernel, count),
        out_shape=(
            jax.ShapeDtypeStruct((length, width), jnp.bfloat16),
            jax.ShapeDtypeStruct((1, heads * HD), jnp.bfloat16),
        ),
        in_specs=[vmem, vmem],
        out_specs=(hbm, hbm),
        scratch_shapes=[pltpu.SemaphoreType.DMA, pltpu.SemaphoreType.DMA],
        compiler_params=pltpu.CompilerParams(vmem_limit_bytes=24 * 2**20),
    )(got, read)
    rest = pl.pallas_call(
        functools.partial(second_kernel, count),
        out_shape=pltpu.VMEM((LATE * CHUNK, width), jnp.bfloat16),
        in_specs=[vmem, hbm],
        out_specs=vmem,
        scratch_shapes=[pltpu.SemaphoreType.DMA, pltpu.SemaphoreType.DMA],
        compiler_params=pltpu.CompilerParams(
            collective_id=1, has_side_effects=True, vmem_limit_bytes=24 * 2**20
        ),
    )(proj, read)
    cache = pl.pallas_call(
        functools.partial(complete_kernel, count),
        out_shape=jax.ShapeDtypeStruct((length, width), jnp.bfloat16),
        in_specs=[vmem, hbm],
        out_specs=hbm,
        scratch_shapes=[pltpu.SemaphoreType.DMA],
        input_output_aliases={1: 0},
        compiler_params=pltpu.CompilerParams(vmem_limit_bytes=24 * 2**20),
    )(rest, cache)
    return cache.reshape(1, 1, length, width), read


def solution(mesh):
    placed = (P(("gr", "tp"), "sp", None), P(), P(("gr", "tp"), None), P())
    return jax.shard_map(
        local,
        mesh=mesh,
        in_specs=placed,
        out_specs=(P(("gr", "tp"), "sp", None, None), P(("gr", "tp"), None)),
        check_vma=False,
    )
```

```python
import functools

import jax
import jax.numpy as jnp
from jax import lax
from jax.experimental import pallas as pl
from jax.experimental.pallas import tpu as pltpu
from jax.sharding import PartitionSpec as P

KVH = 8
HD = 64


def prefix(shard, axis, combine, identity):
    size, index = (lax.axis_size(axis), lax.axis_index(axis))
    everything = lax.all_gather(shard, axis)
    start = jnp.broadcast_to(jnp.asarray(identity, shard.dtype), shard.shape)

    def hop(k, before):
        at = size - 1 - k
        reached = at > index
        new = combine(before, everything[at])
        return jnp.where(reached, new, before)

    return lax.fori_loop(0, size, hop, start)


def add_terms(earlier, later):
    return earlier + later


def finish(contribution):
    return lax.psum(contribution, "sp").astype(jnp.bfloat16)


def local_plain(tokens, kv_weight, queries, score_offset):
    seq_count, pos_rows, model_width = tokens.shape
    features = kv_weight.shape[1]
    slot_count = lax.axis_size("sp")
    blocks = slot_count // seq_count
    block_width = features // blocks
    half_blocks = blocks // 2
    heads = score_offset.shape[0]
    group_size = heads // KVH
    per_block = block_width // HD
    projected = jnp.einsum(
        "spd,dcw->scpw",
        tokens,
        kv_weight.reshape(model_width, blocks, block_width),
        preferred_element_type=jnp.float32,
    ).astype(jnp.bfloat16)
    received = lax.all_to_all(
        projected.reshape(slot_count, pos_rows, block_width),
        "sp",
        split_axis=0,
        concat_axis=1,
        tiled=True,
    )
    length = received.shape[1]
    cache = received.reshape(1, 1, length, block_width)
    key_part = projected[:, :half_blocks].reshape(seq_count, half_blocks, pos_rows, per_block, HD)
    value_part = (
        projected[:, half_blocks:]
        .reshape(seq_count, half_blocks, pos_rows, per_block, HD)
        .astype(jnp.float32)
    )
    query_heads = queries.reshape(seq_count, half_blocks, per_block, group_size, HD)
    offsets = score_offset.reshape(half_blocks, per_block, group_size)
    logits = jnp.einsum(
        "scvgd,scpvd->scvgp", query_heads, key_part, preferred_element_type=jnp.float32
    )
    logits = logits * HD ** (-0.5) + offsets[None, :, :, :, None]
    keep_log = jax.nn.log_sigmoid(-logits)
    between = lax.cumsum(keep_log, axis=4, reverse=True) - keep_log
    totals = jnp.sum(keep_log, axis=4)
    later_keep = prefix(totals, "sp", add_terms, jnp.zeros_like(totals))
    weights = jnp.exp(jax.nn.log_sigmoid(logits) + between + later_keep[..., None])
    weighted = jnp.einsum("scvgp,scpvd->scvgd", weights, value_part)
    contribution = weighted.reshape(seq_count, heads * HD)
    return (cache, finish(contribution))


CHUNK = 128
FIRST = 64
EARLY = 4
SLICES = 2
LATE = 12
VMEM_LIMIT = 51 * 2**20
LANES = 128
MESH = pl.DeviceIdType.MESH


def is_late(count):
    me = lax.axis_index("sp")
    in_middle = jnp.logical_or(me == count // 2 - 1, me == count // 2)
    return jnp.logical_and(in_middle, lax.rem(lax.axis_index("tp"), 2) == 1)


def exchange_kernel(
    count,
    tok_hbm,
    w_hbm,
    q_hbm,
    off_hbm,
    recv,
    read_ref,
    proj,
    tok,
    wts,
    q_ref,
    off_ref,
    qbig,
    part,
    whole,
    outer_part,
    other_part,
    inner_whole,
    load_sem,
    send_sem,
    recv_sem,
    psend_sem,
    precv_sem,
    ready,
):
    me = lax.axis_index("sp")
    rows = tok.shape[0]
    model_width = tok.shape[1]
    width = wts.shape[2]
    chunks = rows // CHUNK
    heads = off_ref.shape[1]
    group = heads // KVH
    half = count // 2
    depth = model_width // SLICES
    sides = width // LANES

    lower = me < half
    inner = jnp.where(lower, half - 1, half)
    mate = jnp.where(lower, half, half - 1)
    is_inner = me == inner
    inward = jnp.where(lower, me + 1, me - 1)
    outward = jnp.where(lower, me - 1, me + 1)
    has_outer = jnp.logical_and(me > 0, me < count - 1)

    def dest(j):
        if j == count - 1:
            return me
        down = count - 1 - j
        return jnp.where(
            lower,
            jnp.where(down > me, down, down - 1),
            jnp.where(j < me, j, j + 1),
        )

    def span(c):
        return pl.ds(pl.multiple_of(c * CHUNK, CHUNK), CHUNK)

    def tok_copy(c):
        sem = load_sem.at[lax.rem(c, EARLY)]
        return pltpu.make_async_copy(tok_hbm.at[span(c), :], tok.at[span(c), :], sem)

    def w_copy(d):
        at = pl.ds(pl.multiple_of(d * width, width), width)
        return pltpu.make_async_copy(w_hbm.at[:, at], wts.at[d], load_sem.at[EARLY + 2])

    def slice_copy(side, k):
        at = pl.ds(pl.multiple_of(mate * width + side * LANES, LANES), LANES)
        return pltpu.make_async_copy(
            w_hbm.at[pl.ds(k * depth, depth), at],
            wts.at[mate, pl.ds(k * depth, depth), pl.ds(side * LANES, LANES)],
            load_sem.at[EARLY + side * SLICES + k],
        )

    def rows_copy(d, start, size, columns=pl.ds(0, width)):
        here = pl.ds(pl.multiple_of(start, FIRST), size)
        there = pl.ds(pl.multiple_of(me * rows + start, FIRST), size)
        return pltpu.make_async_remote_copy(
            src_ref=proj.at[d, here, columns],
            dst_ref=recv.at[there, columns],
            send_sem=send_sem,
            recv_sem=recv_sem,
            device_id={"sp": d},
            device_id_type=MESH,
        )

    def block_copy(d, c):
        return rows_copy(d, c * CHUNK, CHUNK)

    def top_copy(start, size, sem):
        at = pl.ds(start, size)
        return pltpu.make_async_copy(tok_hbm.at[at, :], tok.at[at, :], load_sem.at[sem])

    barrier = pltpu.get_barrier_semaphore()

    @pl.when(is_inner)
    def _():
        pl.semaphore_signal(barrier, inc=1, device_id={"sp": mate}, device_id_type=MESH)

    first_at, rest_at = rows - FIRST, rows - CHUNK
    first_copy = top_copy(first_at, FIRST, EARLY + sides * SLICES)
    rest_copy = top_copy(rest_at, CHUNK - FIRST, (chunks - 1) % EARLY)
    first_copy.start()
    for side in range(sides):
        for k in range(SLICES):
            slice_copy(side, k).start()
    rest_copy.start()
    tok_copy(chunks - 2).start()

    small_copies = [
        pltpu.make_async_copy(q_hbm, q_ref, load_sem.at[EARLY]),
        pltpu.make_async_copy(off_hbm, off_ref, load_sem.at[EARLY + 1]),
    ]
    first_copy.wait()
    for side in range(sides):
        lanes = pl.ds(side * LANES, LANES)
        first = jnp.zeros((FIRST, LANES), jnp.float32)
        for k in range(SLICES):
            slice_copy(side, k).wait()
            deep = pl.ds(k * depth, depth)
            first = first + jnp.dot(
                tok[pl.ds(first_at, FIRST), deep],
                wts[mate, deep, lanes],
                preferred_element_type=jnp.float32,
            )
        proj[mate, pl.ds(first_at, FIRST), lanes] = first.astype(jnp.bfloat16)
        if side == 0:
            for early_chunk in range(2, EARLY):
                tok_copy(chunks - 1 - early_chunk).start()
            pl.semaphore_wait(barrier, 1)
        else:
            for copy in small_copies if side == 1 else ():
                copy.start()
        rows_copy(mate, first_at, FIRST, lanes).start()
    for j in range(count):
        if j != half - 1:
            w_copy(dest(j)).start()

    for d in range(count):
        same = (d < half) == lower

        @pl.when(jnp.logical_and(is_inner, jnp.logical_and(same, d != me)))
        def _():
            pl.semaphore_signal(barrier, inc=1, device_id={"sp": d}, device_id_type=MESH)

    @pl.when(jnp.logical_not(is_inner))
    def _():
        for d in (half - 1, half):
            pl.semaphore_signal(ready, inc=1, device_id={"sp": d}, device_id_type=MESH)

    rest_copy.wait()
    proj[mate, pl.ds(rest_at, CHUNK - FIRST), :] = jnp.dot(
        tok[pl.ds(rest_at, CHUNK - FIRST), :], wts[mate], preferred_element_type=jnp.float32
    ).astype(jnp.bfloat16)

    def early(k, carry):
        c = chunks - 1 - k
        tok_copy(c).wait()

        @pl.when(k == 1)
        def _():
            rows_copy(mate, rest_at, CHUNK - FIRST).start()

        proj[mate, span(c), :] = jnp.dot(
            tok[span(c), :], wts[mate], preferred_element_type=jnp.float32
        ).astype(jnp.bfloat16)

        @pl.when(k > 1)
        def _():
            block_copy(mate, c + 1).start()

        return carry

    lax.fori_loop(1, EARLY, early, 0)
    for copy in small_copies:
        copy.wait()

    q_rows = []
    for h in range(heads):
        pair = q_ref[:, h // 2 * LANES : (h // 2 + 1) * LANES].astype(jnp.float32)
        q_rows.append(pair if h % 2 == h // group % 2 else pltpu.roll(pair, HD, axis=1))
    spread = jnp.concatenate(
        [jnp.concatenate(q_rows, axis=0)] * (KVH * HD // LANES), axis=1
    )
    diagonal = lax.broadcasted_iota(jnp.int32, (heads, LANES), 0) == lax.broadcasted_iota(
        jnp.int32, (heads, LANES), 1
    )

    def to_column(row):
        return jnp.sum(
            jnp.where(diagonal, jnp.broadcast_to(row, (heads, LANES)), 0.0), axis=1, keepdims=True
        )

    def to_row(column):
        return jnp.sum(
            jnp.where(diagonal, jnp.broadcast_to(column, (heads, LANES)), 0.0),
            axis=0,
            keepdims=True,
        )

    square = (heads, heads)
    offsets = jnp.sum(
        jnp.where(
            diagonal[:, :heads], jnp.broadcast_to(off_ref[...], square), 0.0
        ),
        axis=1,
        keepdims=True,
    )
    column = lax.broadcasted_iota(jnp.int32, spread.shape, 1) // HD
    row = lax.broadcasted_iota(jnp.int32, spread.shape, 0) // group
    mine = column == row
    qbig[...] = jnp.where(mine, spread, 0.0).astype(jnp.bfloat16)
    earlier = lax.broadcasted_iota(jnp.int32, (CHUNK, CHUNK), 1)
    later = lax.broadcasted_iota(jnp.int32, (CHUNK, CHUNK), 0)
    after = jnp.where(later > earlier, 1.0, 0.0).astype(jnp.bfloat16)

    block_copy(mate, chunks - EARLY).start()

    @pl.when(is_inner)
    def _():
        pl.semaphore_wait(ready, count - 2)

    for d in range(count):
        same = (d < half) == lower

        @pl.when(jnp.logical_and(is_inner, jnp.logical_and(same, d != me)))
        def _():
            pl.semaphore_signal(ready, inc=1, device_id={"sp": d}, device_id_type=MESH)

    @pl.when(jnp.logical_not(is_inner))
    def _():
        pl.semaphore_wait(ready, 1)

    others = pl.ds(0, count - 1)
    pltpu.make_async_copy(wts.at[others], wts.at[others], load_sem.at[EARLY + 2]).wait()

    def deferred(d):
        crosses = (d < half) != lower
        return jnp.logical_or(
            d == mate, jnp.logical_and(jnp.logical_not(crosses), jnp.logical_not(has_outer))
        )

    def step(i, state):
        kept, total = state
        c = chunks - 1 - i
        at = span(c)

        @pl.when(i >= EARLY)
        def _():
            tok_copy(c).wait()

        @pl.when(i + EARLY < chunks)
        def _():
            tok_copy(c - EARLY).start()

        before = None
        for j in range(count):
            d = dest(j)
            if j == half - 1:

                @pl.when(i >= EARLY)
                def _():
                    proj[mate, at, :] = jnp.dot(
                        tok[at, :], wts[mate], preferred_element_type=jnp.float32
                    ).astype(jnp.bfloat16)

            else:

                block = jnp.dot(
                    tok[at, :], wts[d], preferred_element_type=jnp.float32
                ).astype(jnp.bfloat16)
                proj[d, at, :] = block
                if j == count - 1:
                    own = pl.ds(pl.multiple_of(me * rows + c * CHUNK, CHUNK), CHUNK)
                    recv[own, :] = block
            if before is not None:
                send = before

                @pl.when(jnp.logical_not(deferred(send)))
                def _():
                    block_copy(send, c).start()

            before = None if j == half - 1 else d

        logits = jnp.zeros((heads, CHUNK), jnp.float32)
        for b in range(half):
            logits = logits + lax.dot_general(
                qbig[:, b * width : (b + 1) * width],
                proj[b, at, :],
                (((1,), (1,)), ((), ())),
                preferred_element_type=jnp.float32,
            )
        logits = logits * HD ** (-0.5) + offsets
        keep = -(jnp.maximum(logits, 0.0) + jnp.log1p(jnp.exp(-jnp.abs(logits))))
        high = keep.astype(jnp.bfloat16)
        rest = keep - high.astype(jnp.float32)
        mid = rest.astype(jnp.bfloat16)
        low = (rest - mid.astype(jnp.float32)).astype(jnp.bfloat16)
        sums = jnp.dot(
            jnp.concatenate([high, mid, low], axis=0), after, preferred_element_type=jnp.float32
        )
        between = sums[:heads] + sums[heads : 2 * heads] + sums[2 * heads :]
        weight = jnp.exp(logits + keep + between + kept)
        weight_high = weight.astype(jnp.bfloat16)
        weight_low = (weight - weight_high.astype(jnp.float32)).astype(jnp.bfloat16)
        both = jnp.concatenate([weight_high, weight_low], axis=0)
        summed = jnp.concatenate(
            [
                jnp.dot(both, proj[half + b, at, :], preferred_element_type=jnp.float32)
                for b in range(half)
            ],
            axis=1,
        )
        total = total + summed[:heads] + summed[heads:]
        kept = kept + jnp.sum(keep, axis=1, keepdims=True)
        return kept, total

    kept, total = lax.fori_loop(
        0,
        chunks,
        step,
        (jnp.zeros((heads, 1), jnp.float32), jnp.zeros((heads, KVH * HD), jnp.float32)),
    )

    pairs = heads // 2
    left_lanes = lax.broadcasted_iota(jnp.int32, (heads, LANES), 1) < HD
    left_head = lax.broadcasted_iota(jnp.int32, (heads, LANES), 0) // group % 2 == 0

    def pack(x):
        x = jnp.where(left_lanes == left_head, x, 0.0)
        return jnp.concatenate(
            [
                x[2 * g * group : (2 * g + 1) * group] + x[(2 * g + 1) * group : (2 * g + 2) * group]
                for g in range(KVH // 2)
            ],
            axis=0,
        )

    def join(early_sums, early_row, late_sums, late_row):
        spread_keep = jnp.broadcast_to(to_column(late_row), (heads, LANES))
        return late_sums + jnp.exp(pack(spread_keep)) * early_sums, early_row + late_row

    def join_sides(sums, row, other_sums, other_row, own_late):
        return join(
            jnp.where(own_late, other_sums, sums),
            jnp.where(own_late, other_row, row),
            jnp.where(own_late, sums, other_sums),
            jnp.where(own_late, row, other_row),
        )

    total = jnp.where(mine, total, 0.0)
    folded = total[:, :LANES]
    for g in range(1, KVH * HD // LANES):
        folded = folded + total[:, g * LANES : (g + 1) * LANES]
    part[:pairs] = pack(folded)
    part[pairs:] = to_row(kept)

    def part_copy(src, dst, to, sent, got):
        return pltpu.make_async_remote_copy(
            src_ref=src,
            dst_ref=dst,
            send_sem=psend_sem.at[sent],
            recv_sem=precv_sem.at[got],
            device_id={"sp": to},
            device_id_type=MESH,
        )

    def send_deferred(start, stop):
        @pl.loop(start, stop)
        def _(i):
            for j in range(count - 1):
                d = dest(j)
                ahead = i >= EARLY if j == half - 1 else True

                @pl.when(jnp.logical_and(deferred(d), ahead))
                def _():
                    block_copy(d, chunks - 1 - i).start()

    late = is_late(count)
    stop = jnp.where(late, chunks - LATE, chunks)
    pause = jnp.minimum(2 * EARLY, stop)

    @pl.when(has_outer)
    def _():
        send_deferred(EARLY, pause)
        part_copy(part, outer_part, inward, 0, 0).wait_recv()
        sums, row = join_sides(
            part[:pairs], part[pairs:], outer_part[:pairs], outer_part[pairs:], lower
        )
        part[:pairs] = sums
        part[pairs:] = row

    @pl.when(jnp.logical_not(has_outer))
    def _():
        send_deferred(0, EARLY)

    @pl.when(is_inner)
    def _():
        part_copy(part, other_part, mate, 0, 1).start()

    @pl.when(jnp.logical_not(is_inner))
    def _():
        part_copy(part, outer_part, inward, 0, 0).start()

    @pl.when(has_outer)
    def _():
        send_deferred(pause, stop)

    @pl.when(jnp.logical_not(has_outer))
    def _():
        send_deferred(EARLY, chunks)

    @pl.when(is_inner)
    def _():
        part_copy(part, other_part, mate, 0, 1).wait_recv()
        sums, row = join_sides(
            part[:pairs],
            part[pairs:],
            other_part[:pairs],
            other_part[pairs:],
            jnp.logical_not(lower),
        )
        whole[:pairs] = sums
        whole[pairs:] = row

    @pl.when(jnp.logical_not(is_inner))
    def _():
        part_copy(whole, inner_whole, outward, 1, 1).wait_recv()
        whole[...] = inner_whole[...]

    packed = whole[:pairs]
    turned = pltpu.roll(packed, HD, axis=1)
    low_half = lax.broadcasted_iota(jnp.int32, (1, LANES), 1) < HD

    def head_at(h, side):
        source = packed if h // group % 2 == side else turned
        at = h // group // 2 * group + h % group
        return source[at : at + 1]

    for m in range(pairs):
        piece = jnp.where(low_half, head_at(2 * m, 0), head_at(2 * m + 1, 1))
        read_ref[:, m * LANES : (m + 1) * LANES] = piece.astype(read_ref.dtype)

    @pl.when(has_outer)
    def _():
        out = part_copy(whole, inner_whole, outward, 1, 1)
        out.start()
        out.wait_send()

    part_copy(part, other_part, mate, 0, 1).wait_send()
    def finish_blocks(size):
        foreign = pl.ds(0, size)
        blocks = pltpu.make_async_remote_copy(
            src_ref=recv.at[foreign, :],
            dst_ref=recv.at[foreign, :],
            send_sem=send_sem,
            recv_sem=recv_sem,
            device_id={"sp": mate},
            device_id_type=MESH,
        )
        blocks.wait_send()
        blocks.wait_recv()

    @pl.when(late)
    def _():
        finish_blocks((count - 1) * rows - LATE * CHUNK)

    @pl.when(jnp.logical_not(late))
    def _():
        finish_blocks((count - 1) * rows)


def second_kernel(count, proj, _, rest, send_sem, recv_sem):
    me = lax.axis_index("sp")
    mate = jnp.where(me < count // 2, count // 2, count // 2 - 1)

    @pl.when(is_late(count))
    def _():
        barrier = pltpu.get_barrier_semaphore()
        pl.semaphore_signal(barrier, inc=1, device_id={"sp": mate}, device_id_type=MESH)
        pl.semaphore_wait(barrier, 1)
        copy = pltpu.make_async_remote_copy(
            src_ref=proj.at[mate, pl.ds(0, LATE * CHUNK), :],
            dst_ref=rest,
            send_sem=send_sem,
            recv_sem=recv_sem,
            device_id={"sp": mate},
            device_id_type=MESH,
        )
        copy.start()
        copy.wait()


def place_kernel(count, got, read, cache, read_out, sem, read_sem):
    rows = got.shape[0] // count
    me = lax.axis_index("sp")
    mate = jnp.where(me < count // 2, count // 2, count // 2 - 1)
    late = is_late(count)

    def copy(start, size):
        at = pl.ds(pl.multiple_of(start, CHUNK), size)
        return pltpu.make_async_copy(got.at[at, :], cache.at[at, :], sem)

    read_copy = pltpu.make_async_copy(read, read_out, read_sem)
    for d in range(count):

        @pl.when(jnp.logical_and(late, d == mate))
        def _():
            copy(d * rows + LATE * CHUNK, rows - LATE * CHUNK).start()

        @pl.when(jnp.logical_not(jnp.logical_and(late, d == mate)))
        def _():
            copy(d * rows, rows).start()

    read_copy.start()
    read_copy.wait()

    @pl.when(late)
    def _():
        copy(0, count * rows - LATE * CHUNK).wait()

    @pl.when(jnp.logical_not(late))
    def _():
        copy(0, count * rows).wait()


def complete_kernel(count, rest, _, cache, sem):
    rows = cache.shape[0] // count
    me = lax.axis_index("sp")
    mate = jnp.where(me < count // 2, count // 2, count // 2 - 1)

    @pl.when(is_late(count))
    def _():
        at = pl.ds(pl.multiple_of(mate * rows, CHUNK), LATE * CHUNK)
        copy = pltpu.make_async_copy(rest, cache.at[at, :], sem)
        copy.start()
        copy.wait()


def local(tokens, kv_weight, queries, score_offset):
    seq_count, rows, model_width = tokens.shape
    features = kv_weight.shape[1]
    heads = score_offset.shape[0]
    count = lax.axis_size("sp")
    width = features // (count // seq_count)
    fits = (
        seq_count == 1
        and count % 2 == 0
        and count > 2
        and width % LANES == 0
        and rows % CHUNK == 0
        and rows >= (EARLY + LATE) * CHUNK
        and model_width % (SLICES * LANES) == 0
        and features == 2 * KVH * HD
        and 2 * HD == LANES
        and heads % KVH == 0
        and rows // CHUNK % EARLY == 0
        and heads <= LANES
    )
    if not fits:
        return local_plain(tokens, kv_weight, queries, score_offset)
    length = rows * count
    vmem = pl.BlockSpec(memory_space=pltpu.VMEM)
    hbm = pl.BlockSpec(memory_space=pltpu.HBM)
    got, read, proj = pl.pallas_call(
        functools.partial(exchange_kernel, count),
        out_shape=(
            pltpu.VMEM((length, width), jnp.bfloat16),
            pltpu.VMEM((1, heads * HD), jnp.bfloat16),
            pltpu.VMEM((count, rows, width), jnp.bfloat16),
        ),
        in_specs=[hbm, hbm, hbm, hbm],
        out_specs=(vmem, vmem, vmem),
        scratch_shapes=[
            pltpu.VMEM((rows, model_width), jnp.bfloat16),
            pltpu.VMEM((count, model_width, width), jnp.bfloat16),
            pltpu.VMEM((1, heads * HD), jnp.bfloat16),
            pltpu.VMEM((1, heads), jnp.float32),
            pltpu.VMEM((heads, KVH * HD), jnp.bfloat16),
            *[pltpu.VMEM((heads // 2 + 1, LANES), jnp.float32)] * 5,
            pltpu.SemaphoreType.DMA((EARLY + width // LANES * SLICES + 1,)),
            pltpu.SemaphoreType.DMA,
            pltpu.SemaphoreType.DMA,
            pltpu.SemaphoreType.DMA((2,)),
            pltpu.SemaphoreType.DMA((2,)),
            pltpu.SemaphoreType.REGULAR,
        ],
        compiler_params=pltpu.CompilerParams(
            collective_id=0, has_side_effects=True, vmem_limit_bytes=VMEM_LIMIT
        ),
    )(
        tokens.reshape(rows, model_width),
        kv_weight,
        queries,
        score_offset.reshape(1, heads),
    )
    cache, read = pl.pallas_call(
        functools.partial(place_kernel, count),
        out_shape=(
            jax.ShapeDtypeStruct((length, width), jnp.bfloat16),
            jax.ShapeDtypeStruct((1, heads * HD), jnp.bfloat16),
        ),
        in_specs=[vmem, vmem],
        out_specs=(hbm, hbm),
        scratch_shapes=[pltpu.SemaphoreType.DMA, pltpu.SemaphoreType.DMA],
        compiler_params=pltpu.CompilerParams(vmem_limit_bytes=24 * 2**20),
    )(got, read)
    rest = pl.pallas_call(
        functools.partial(second_kernel, count),
        out_shape=pltpu.VMEM((LATE * CHUNK, width), jnp.bfloat16),
        in_specs=[vmem, hbm],
        out_specs=vmem,
        scratch_shapes=[pltpu.SemaphoreType.DMA, pltpu.SemaphoreType.DMA],
        compiler_params=pltpu.CompilerParams(
            collective_id=1, has_side_effects=True, vmem_limit_bytes=24 * 2**20
        ),
    )(proj, read)
    cache = pl.pallas_call(
        functools.partial(complete_kernel, count),
        out_shape=jax.ShapeDtypeStruct((length, width), jnp.bfloat16),
        in_specs=[vmem, hbm],
        out_specs=hbm,
        scratch_shapes=[pltpu.SemaphoreType.DMA],
        input_output_aliases={1: 0},
        compiler_params=pltpu.CompilerParams(vmem_limit_bytes=24 * 2**20),
    )(rest, cache)
    return cache.reshape(1, 1, length, width), read


def solution(mesh):
    placed = (P(("gr", "tp"), "sp", None), P(), P(("gr", "tp"), None), P())
    return jax.shard_map(
        local,
        mesh=mesh,
        in_specs=placed,
        out_specs=(P(("gr", "tp"), "sp", None, None), P(("gr", "tp"), None)),
        check_vma=False,
    )
```
